256 devices in a mesh: row: 32 (over z, x), col: 8 (over y, core).
Axes of the slice: x: 4, y: 4, z: 8, core: 2. Of those that a mesh axis runs over, the one named last changes fastest.
Arguments:
- tokens: bfloat16 [8192, 2048], P('row'), may hold values from -6 to 6
- norm_gain: float32 [2048], replicated, may hold values from 0.5 to 1.5
- first_gate: bfloat16 [2048, 1024], P(None, 'col'), may hold values from -0.125 to 0.125
- second_gate: bfloat16 [2048, 1024], P(None, 'col'), may hold values from -0.125 to 0.125
- value_weight: bfloat16 [2048, 1024], P(None, 'col'), may hold values from -0.125 to 0.125
- short_weight: bfloat16 [3, 3, 1024], P(None, None, 'col'), may hold values from -3.5 to 3.5
- short_bias: float32 [3, 1024], P(None, 'col'), may hold values from -2 to 2
- embed_weight: float32 [33, 64], replicated, may hold values from -1 to 1
- embed_bias: float32 [64], replicated, may hold values from -3 to 3
- inner_weight: float32 [64, 64], replicated, may hold values from -0.75 to 0.75
- inner_bias: float32 [64], replicated, may hold values from -3 to 3
- filter_freq: float32 [64], replicated, may hold values from 0.5 to 1.5
- filter_weight: float32 [2, 2, 64, 1024], P(None, None, None, ('col', 'row')), may hold values from -0.0234375 to 0.0234375
- filter_skip: float32 [2, 1024], P(None, ('col', 'row')), may hold values from -3 to 3
- output_gain: float32 [1024], P('col'), may hold values from 0.5 to 1.5
- output_weight: bfloat16 [1024, 2048], replicated, may hold values from -0.1875 to 0.1875
Outputs:
- mixed_output: bfloat16 [8192, 2048], P(('row', 'col'))
The draws below stay inside these ranges and needn't reach their ends.
All inputs are finite; a program needn't handle non-finite values.
Results may differ from the reference program's by a relative error of at most 0.01.
Values may be sent and summed in bfloat16 or wider, within the bound.
A program may use at most 64 MiB of HBM per device.

```python
import math
import jax
import jax.numpy as jnp
from jax import lax

MODEL_WIDTH = 2048
CHANNELS = 1024
GROUPS = 8
SHORT = 3
FREQ_BANDS = 16
FEATURES = 33
FILTER_HIDDEN = 64
SEQ_LEN = 8192


def shard_levels(key, dims, cuts, smallest, top_value):
    loudness = 1.0
    for dim, blocks in cuts:
        draws = jax.random.uniform(jax.random.fold_in(jax.random.fold_in(key, 6), dim), (blocks,), jnp.float32, smallest / len(cuts), top_value / len(cuts))
        loudness = loudness * jnp.repeat(jnp.exp(draws), dims[dim] // blocks).reshape((-1,) + (1,) * (len(dims) - 1 - dim))
    return loudness


def scatter_about(stream_key, shape, deviation, limit, cuts=(), held_as=jnp.bfloat16):
    array = deviation * jax.random.normal(stream_key, shape, jnp.float32)
    if cuts:
        array = array * shard_levels(stream_key, shape, cuts, -0.22, 0.18)
    return jnp.clip(array, -limit, limit).astype(held_as)


def setup_inputs(seed: int = 0) -> dict:
    key_of = jax.random.split(jax.random.key(seed), 17)
    return {
        "tokens": scatter_about(key_of[0], (SEQ_LEN, MODEL_WIDTH), 1.0, 6.0, ((0, 32),)),
        "norm_gain": jnp.clip(1.0 + 0.1 * jax.random.normal(key_of[1], (MODEL_WIDTH,), jnp.float32), 0.5, 1.5),
        "first_gate": scatter_about(key_of[2], (MODEL_WIDTH, CHANNELS), MODEL_WIDTH ** -0.5, 0.125, ((1, 8),)),
        "second_gate": scatter_about(key_of[3], (MODEL_WIDTH, CHANNELS), MODEL_WIDTH ** -0.5, 0.125, ((1, 8),)),
        "value_weight": scatter_about(key_of[4], (MODEL_WIDTH, CHANNELS), MODEL_WIDTH ** -0.5, 0.125, ((1, 8),)),
        "short_weight": scatter_about(key_of[5], (3, SHORT, CHANNELS), SHORT ** -0.5, 3.5, ((2, 8),)),
        "short_bias": scatter_about(key_of[6], (3, CHANNELS), 0.3, 2.0, ((1, 8),), jnp.float32),
        "embed_weight": scatter_about(key_of[7], (FEATURES, FILTER_HIDDEN), FEATURES ** -0.5, 1.0, (), jnp.float32),
        "embed_bias": scatter_about(key_of[8], (FILTER_HIDDEN,), 0.5, 3.0, (), jnp.float32),
        "inner_weight": scatter_about(key_of[9], (FILTER_HIDDEN, FILTER_HIDDEN), FILTER_HIDDEN ** -0.5, 0.75, (), jnp.float32),
        "inner_bias": scatter_about(key_of[10], (FILTER_HIDDEN,), 0.5, 3.0, (), jnp.float32),
        "filter_freq": jnp.clip(1.0 + 0.1 * jax.random.normal(key_of[11], (FILTER_HIDDEN,), jnp.float32), 0.5, 1.5),
        "filter_weight": scatter_about(key_of[12], (2, 2, FILTER_HIDDEN, CHANNELS), (FILTER_HIDDEN * SEQ_LEN // 8) ** -0.5, 0.0234375, ((3, 256),), jnp.float32),
        "filter_skip": scatter_about(key_of[13], (2, CHANNELS), 0.5, 3.0, ((1, 256),), jnp.float32),
        "output_gain": jnp.clip(1.0 + 0.1 * jax.random.normal(key_of[14], (CHANNELS,), jnp.float32), 0.5, 1.5),
        "output_weight": scatter_about(key_of[15], (CHANNELS, MODEL_WIDTH), CHANNELS ** -0.5, 0.1875),
    }


HIGHEST = lax.Precision.HIGHEST
NORM_EPS = 1e-06
DECAY_TARGET = 0.01
FAST_SPAN = 0.3
SLOW_SPAN = 1.5

def position_features(length):
    position_ramp = jnp.linspace(0.0, 1.0, length, dtype=jnp.float32)[:, None]
    angles = 2.0 * math.pi * jnp.arange(length, dtype=jnp.float32)[:, None] / length
    band_freqs = jnp.linspace(0.0001, FREQ_BANDS - 1, FREQ_BANDS, dtype=jnp.float32)[None, :]
    features = jnp.concatenate([position_ramp, jnp.cos(band_freqs * angles), -jnp.sin(band_freqs * angles)], axis=1)
    return (position_ramp, features)

def filter_hidden(length, embed_weight, embed_bias, inner_weight, inner_bias, filter_freq):
    position_ramp, features = position_features(length)
    hidden = jnp.sin(filter_freq * (jnp.dot(features, embed_weight, precision=HIGHEST) + embed_bias))
    hidden = jnp.sin(filter_freq * (jnp.dot(hidden, inner_weight, precision=HIGHEST) + inner_bias))
    return (position_ramp, hidden)

def decay_rates():
    fastest = math.log(DECAY_TARGET) / FAST_SPAN
    slowest = math.log(DECAY_TARGET) / SLOW_SPAN
    return jnp.abs(jnp.linspace(slowest, fastest, CHANNELS, dtype=jnp.float32))

def short_filter(padded, weights, bias_row, length):
    result = bias_row.astype(jnp.float32)
    for tap_index in range(weights.shape[0]):
        result = result + padded[tap_index:tap_index + length].astype(jnp.float32) * weights[tap_index].astype(jnp.float32)
    return result

def two_sided(signal, forward, backward, skip_gain):
    length = signal.shape[0]
    circular_taps = jnp.concatenate([forward, jnp.zeros_like(forward[:1]), backward[:0:-1]], axis=0)
    spectrum = jnp.fft.rfft(signal, n=2 * length, axis=0) * jnp.fft.rfft(circular_taps, axis=0)
    return jnp.fft.irfft(spectrum, n=2 * length, axis=0)[:length] + signal * skip_gain

def reference(tokens, norm_gain, first_gate, second_gate, value_weight, short_weight, short_bias, embed_weight, embed_bias, inner_weight, inner_bias, filter_freq, filter_weight, filter_skip, output_gain, output_weight):
    widened = tokens.astype(jnp.float32)
    normed = (widened * lax.rsqrt(lax.optimization_barrier(jnp.mean(widened * widened, axis=1, keepdims=True)) + NORM_EPS) * norm_gain).astype(jnp.bfloat16)
    gate_first = jnp.dot(normed, first_gate, preferred_element_type=jnp.float32).astype(jnp.bfloat16)
    gate_second = jnp.dot(normed, second_gate, preferred_element_type=jnp.float32).astype(jnp.bfloat16)
    gate_value = jnp.dot(normed, value_weight, preferred_element_type=jnp.float32).astype(jnp.bfloat16)
    length = tokens.shape[0]
    position_ramp, hidden = filter_hidden(length, embed_weight, embed_bias, inner_weight, inner_bias, filter_freq)
    group_width = CHANNELS // GROUPS
    half_width = SHORT // 2

    def blocks(matrix):
        split = matrix.reshape(matrix.shape[:-1] + (GROUPS, group_width))
        return jnp.moveaxis(split, -2, 0)

    def one_block(pieces):
        first_block, second_block, value_block, weight_block, bias_block, filter_block, skip_block, decay_block, gain_block = pieces
        window = jnp.exp(-position_ramp * decay_block[None, :])
        smoothed = []
        for branch, source in enumerate((first_block, second_block, value_block)):
            padded = jnp.pad(source.astype(jnp.float32), ((half_width, SHORT - 1 - half_width), (0, 0)))
            smoothed.append(short_filter(padded, weight_block[branch], bias_block[branch], length))
        signal = smoothed[2]
        for order_index in range(2):
            forward = jnp.dot(hidden, filter_block[order_index, 0], precision=HIGHEST) * window
            backward = jnp.dot(hidden, filter_block[order_index, 1], precision=HIGHEST) * window
            signal = smoothed[order_index] * two_sided(signal, forward, backward, skip_block[order_index])
        scaled = signal * lax.rsqrt(lax.optimization_barrier(jnp.mean(signal * signal, axis=1, keepdims=True)) + NORM_EPS)
        return (scaled * gain_block).astype(jnp.bfloat16)
    normed_blocks = lax.map(one_block, (blocks(gate_first), blocks(gate_second), blocks(gate_value), blocks(short_weight), blocks(short_bias), blocks(filter_weight), blocks(filter_skip), blocks(decay_rates()), blocks(output_gain)))
    mixed = jnp.moveaxis(normed_blocks, 0, 1).reshape(length, CHANNELS)
    return jnp.dot(mixed, output_weight, preferred_element_type=jnp.float32).astype(jnp.bfloat16)
```

```python
import functools
import math

import jax
import jax.numpy as jnp
import numpy as np
from jax import lax
from jax.experimental import pallas as pl
from jax.experimental.pallas import tpu as pltpu
from jax.sharding import PartitionSpec as P

CHANNELS = 1024
FREQ_BANDS = 16
FEATURES = 33
NORM_EPS = 1e-06
DECAY_TARGET = 0.01
FAST_SPAN = 0.3
SLOW_SPAN = 1.5
LANES = 128
OWN = 4
FEATURE_ROWS = 48
BF16 = jnp.bfloat16
F32 = jnp.float32

SIN_COEFS = (
    6.283185280154403,
    -41.34168061334532,
    81.60247636883796,
    -76.5811726421402,
    39.75982706857711,
)


def fast_tables(length):
    total = 2 * length
    majors = length // LANES
    n1 = np.arange(majors)
    k1 = np.arange(majors) + 0.5
    angle = 2.0 * np.pi * np.outer(k1, n1) / (2 * majors)
    eye = np.eye(OWN)
    inner = np.concatenate([np.kron(np.cos(angle), eye), np.kron(-np.sin(angle), eye)], 0)
    inner_back = inner.T * (2.0 / total)
    n2 = np.arange(LANES)
    turn = np.repeat(2.0 * np.pi * np.outer(k1, n2) / total, OWN, axis=0)
    twiddle = np.stack([np.cos(turn), np.sin(turn)])
    phase = 2.0 * np.pi * (np.outer(n2, n2) % LANES) / LANES
    c, s = np.cos(phase), np.sin(phase)
    outer = np.block([[c, -s], [s, c]])
    ramp = np.linspace(0.0, 1.0, length)
    angles = 2.0 * np.pi * np.arange(length) / length
    bands = np.linspace(0.0001, FREQ_BANDS - 1, FREQ_BANDS)[:, None]
    feats = np.concatenate(
        [ramp[None], np.cos(bands * angles), -np.sin(bands * angles), np.ones((1, length))], 0
    )
    feats = np.pad(feats, ((0, FEATURE_ROWS - feats.shape[0]), (0, 0))).astype(np.float32)
    high = feats.astype(BF16)
    low = (feats - high.astype(np.float32)).astype(BF16)
    return (
        jnp.asarray(inner, BF16),
        jnp.asarray(inner_back, BF16),
        jnp.asarray(twiddle, F32),
        jnp.asarray(outer, BF16),
        jnp.asarray(outer.T, BF16),
        jnp.asarray(np.concatenate([high, low], 0)),
    )


def turn_sin(x):
    d = x - jnp.round(x)
    e = 0.25 - jnp.abs(d)
    q = e * e
    p = SIN_COEFS[4]
    for coef in SIN_COEFS[3::-1]:
        p = coef + q * p
    return e * p


def mm(a, b):
    return jnp.dot(a.astype(BF16), b.astype(BF16), preferred_element_type=F32)


def halves(x):
    high = x.astype(BF16)
    return high, (x - high.astype(F32)).astype(BF16)


def left_three(x):
    high, low = halves(x)
    return jnp.concatenate([high.astype(F32), high.astype(F32), low.astype(F32)], 1).astype(BF16)


def pick(row, start, count):
    shape = (count, row.shape[1])
    want = start + lax.broadcasted_iota(jnp.int32, shape, 0) % OWN
    hit = lax.broadcasted_iota(jnp.int32, shape, 1) == want
    return jnp.sum(jnp.where(hit, row.astype(F32), 0.0), axis=1, keepdims=True)


def column(row):
    count = row.shape[1]
    shape = (count, count)
    hit = lax.broadcasted_iota(jnp.int32, shape, 1) == lax.broadcasted_iota(jnp.int32, shape, 0)
    return jnp.sum(jnp.where(hit, row.astype(F32), 0.0), axis=1, keepdims=True)


def pair(x, y):
    axis = x.ndim - 2
    low = lax.broadcasted_iota(jnp.int32, x.shape, axis) < OWN
    return (
        jnp.where(low, x, pltpu.roll(y, OWN, axis)),
        jnp.where(low, pltpu.roll(x, OWN, axis), y),
    )


SMALL = 11


def fast_kernel(dims, *refs):
    tokens_h, first_h, second_h, value_h, out_w_h = refs[:5]
    small_h = refs[5 : 5 + SMALL]
    inner_h, inner_back_h, twiddle_h, outer_h, outer_back_h, feats_h, out_ref = refs[
        5 + SMALL : 12 + SMALL
    ]
    tokens_v, gates_v, out_w_v = refs[12 + SMALL : 15 + SMALL]
    small_v = refs[15 + SMALL : 15 + 2 * SMALL]
    (
        norm_gain, short_weight, short_bias, embed_weight, embed_bias, inner_weight,
        inner_bias, filter_freq, filter_weight, filter_skip, output_gain,
    ) = small_v
    (
        inner_v, inner_back_v, twiddle_v, outer_v, outer_back_v, feats_v, normed_v,
        send_a, recv_a, send_b, recv_b, send_c, recv_c, second_v, send_h, recv_h,
        taps_v, spectra, embed_pad, load_sem, small_sem, a_sems, b_sems, c_sems,
        send_h_sem, recv_h_sem,
    ) = refs[15 + 2 * SMALL :]
    rows_n, cols_n, block = dims
    length = rows_n * block
    piece = block // cols_n
    row_me = lax.axis_index("row")
    col_me = lax.axis_index("col")
    MESH = pl.DeviceIdType.MESH

    loads = [
        (tokens_h, tokens_v),
        (value_h, gates_v.at[2]),
        (first_h, gates_v.at[0]),
        (second_h, gates_v.at[1]),
        (feats_h, feats_v),
        (inner_h, inner_v),
        (twiddle_h, twiddle_v),
        (outer_h, outer_v),
        (outer_back_h, outer_back_v),
        (inner_back_h, inner_back_v),
        (out_w_h, out_w_v),
    ]
    copies = [
        pltpu.make_async_copy(src, dst, load_sem.at[i]) for i, (src, dst) in enumerate(loads)
    ]
    smalls = [
        pltpu.make_async_copy(src, dst, small_sem.at[i])
        for i, (src, dst) in enumerate(zip(small_h, small_v))
    ]
    copies[0].start()
    smalls[0].start()
    copies[1].start()
    copies[2].start()

    row_peers = [lax.rem(row_me + step, rows_n) for step in range(1, rows_n)]
    col_peers = [lax.rem(col_me + step, cols_n) for step in range(1, cols_n)]
    barrier = pltpu.get_barrier_semaphore()
    for place in [(p, col_me) for p in row_peers] + [(row_me, q) for q in col_peers]:
        pl.semaphore_signal(barrier, inc=1, device_id=place, device_id_type=MESH)

    for copy in smalls[1:] + copies[3:10]:
        copy.start()

    def exchange(send, recv, sems, me, places):
        def copy_of(src, dst, place):
            return pltpu.make_async_remote_copy(
                src_ref=src,
                dst_ref=dst,
                send_sem=sems.at[0],
                recv_sem=sems.at[1],
                device_id=place,
                device_id_type=MESH,
            )

        for peer, place in places:
            copy_of(send.at[peer], recv.at[me], place).start()
        count = len(places)
        return copy_of(send.at[pl.ds(0, count)], recv.at[pl.ds(0, count)], places[0][1])

    copies[0].wait()
    smalls[0].wait()
    gain_row = norm_gain[...]
    chunk = 32
    for start in range(0, block, chunk):
        x = tokens_v[start : start + chunk, :].astype(F32)
        scale = lax.rsqrt(jnp.mean(x * x, axis=1, keepdims=True) + NORM_EPS)
        normed_v[start : start + chunk, :] = (x * scale * gain_row).astype(BF16)

    def project(branch):
        return jnp.dot(normed_v[...], gates_v[branch], preferred_element_type=F32)

    def message(gate):
        turned = gate.T
        even, odd = pair(
            turned[:, :LANES].reshape(rows_n // 2, 2 * OWN, LANES),
            turned[:, LANES:].reshape(rows_n // 2, 2 * OWN, LANES),
        )
        return jnp.stack([even, odd], axis=1).reshape(rows_n, 2 * OWN, LANES)

    copies[1].wait()
    value_part = message(project(2))
    copies[2].wait()
    first_part = message(project(0))
    send_a[...] = jnp.concatenate([value_part, first_part], axis=1).astype(BF16)
    pl.semaphore_wait(barrier, rows_n - 1 + cols_n - 1)
    wait_a = exchange(send_a, recv_a, a_sems, row_me, [(p, (p, col_me)) for p in row_peers])
    recv_a[row_me] = send_a[row_me]

    copies[3].wait()
    gate = project(1).astype(BF16).astype(F32)
    second_v[...] = gate
    send_h[0] = gate[:1]
    send_h[1] = gate[block - 1 :]
    halo = []
    for edge, peer in ((0, row_peers[-1]), (1, row_peers[0])):
        copy = pltpu.make_async_remote_copy(
            src_ref=send_h.at[edge],
            dst_ref=recv_h.at[edge],
            send_sem=send_h_sem.at[edge],
            recv_sem=recv_h_sem.at[edge],
            device_id=(peer, col_me),
            device_id_type=MESH,
        )
        copy.start()
        halo.append(copy)
    copies[10].start()
    for copy in smalls[1:]:
        copy.wait()

    pace = filter_freq[...] * (0.5 / math.pi)
    embed_pad[...] = jnp.zeros_like(embed_pad)
    embed_pad[:FEATURES, :] = embed_weight[...] * pace
    embed_pad[FEATURES : FEATURES + 1, :] = embed_bias[...] * pace - 0.25
    embed_left = left_three(embed_pad[...].T)
    inner_left = left_three((inner_weight[...] * pace).T)
    inner_turn = column(inner_bias[...] * pace - 0.25)
    last = jnp.concatenate([filter_weight[o, d] for o in range(2) for d in range(2)], axis=1)
    last_left = left_three(last.T)
    channels = rows_n * cols_n * OWN
    slowest = math.log(DECAY_TARGET) / SLOW_SPAN
    fastest = math.log(DECAY_TARGET) / FAST_SPAN
    sub = lax.broadcasted_iota(jnp.int32, (2 * OWN, 1), 0)
    channel = ((col_me * rows_n + row_me) * OWN + sub % OWN).astype(F32)
    decay = jnp.abs(slowest + channel * ((fastest - slowest) / (channels - 1)))
    copies[4].wait()
    step_width = 1024
    for start in range(0, length, step_width):
        high = feats_v[:FEATURE_ROWS, start : start + step_width]
        low = feats_v[FEATURE_ROWS:, start : start + step_width]
        hidden = turn_sin(
            jnp.dot(
                embed_left,
                jnp.concatenate([high, low, high], 0),
                preferred_element_type=F32,
            )
        )
        high, low = halves(hidden)
        hidden = turn_sin(
            jnp.dot(
                inner_left,
                jnp.concatenate([high, low, high], 0),
                preferred_element_type=F32,
            )
            + inner_turn
        )
        high, low = halves(hidden)
        taps = jnp.dot(
            last_left, jnp.concatenate([high, low, high], 0), preferred_element_type=F32
        )
        lag = start + lax.broadcasted_iota(jnp.int32, (2 * OWN, step_width), 1)
        window = jnp.exp(-(lag.astype(F32) * (1.0 / (length - 1))) * decay)
        if start == 0:
            window = jnp.where((lag == 0) & (sub >= OWN), 0.0, window)
        for order in range(2):
            x = taps[order * 2 * OWN : (order + 1) * 2 * OWN] * window
            y = pltpu.roll(x, OWN, 0)
            x = jnp.where(sub < OWN, x + y, y - x)
            for m in range(step_width // (2 * LANES)):
                at = 2 * m * LANES
                plus, minus = pair(x[:, at : at + LANES], x[:, at + LANES : at + 2 * LANES])
                spot = (start // (2 * LANES) + m) * 2 * OWN
                lane = 2 * order * LANES
                taps_v[spot : spot + 2 * OWN, lane : lane + LANES] = plus
                taps_v[spot : spot + 2 * OWN, lane + LANES : lane + 2 * LANES] = minus

    for copy in copies[5:8]:
        copy.wait()
    depth = 2 * OWN * rows_n

    def twist(real, imag, sign):
        cos = twiddle_v[0]
        sin = twiddle_v[1] * sign
        return real * cos + imag * sin, imag * cos - real * sin

    part = mm(inner_v[...], taps_v[...])
    for order in range(2):
        for half in range(2):
            lane = (2 * order + half) * LANES
            real, imag = twist(
                part[:depth, lane : lane + LANES], part[depth:, lane : lane + LANES], 1.0
            )
            spot = slice(half * LANES, (half + 1) * LANES)
            spectra[order, :, spot] = mm(
                jnp.concatenate([real, imag], axis=1), outer_v[:, spot]
            )

    shape = (rows_n, 2 * OWN, LANES)
    low_half = lax.broadcasted_iota(jnp.int32, shape, 1) < OWN
    spot = lax.broadcasted_iota(jnp.int32, shape, 2)
    gap = jnp.zeros((1, 2 * OWN, LANES), F32)

    def smooth(x, branch):
        before = pltpu.roll(x, 1, 2)
        other = pltpu.roll(before, OWN, 1)
        earlier = jnp.concatenate([gap, other[:-1]], 0)
        before = jnp.where(spot == 0, jnp.where(low_half, earlier, other), before)
        after = pltpu.roll(x, LANES - 1, 2)
        other = pltpu.roll(after, OWN, 1)
        later = jnp.concatenate([other[1:], gap], 0)
        after = jnp.where(spot == LANES - 1, jnp.where(low_half, other, later), after)
        w = [pick(short_weight[branch, j : j + 1, :], row_me * OWN, 2 * OWN) for j in range(3)]
        bias = pick(short_bias[branch : branch + 1, :], row_me * OWN, 2 * OWN)
        return bias + before * w[0] + x * w[1] + after * w[2]

    for copy in copies[8:10]:
        copy.wait()
    skips = [pick(filter_skip[order : order + 1, :], 0, 2 * OWN) for order in range(2)]

    def convolve(signal, order):
        part = mm(inner_v[...], signal.reshape(depth, LANES))
        real, imag = twist(part[:depth], part[depth:], 1.0)
        spec = mm(jnp.concatenate([real, imag], axis=1), outer_v[...])
        sr, si = spec[:, :LANES], spec[:, LANES:]
        hr, hi = spectra[order, :, :LANES], spectra[order, :, LANES:]
        prod = jnp.concatenate([sr * hr - si * hi, sr * hi + si * hr], axis=1)
        back = mm(prod, outer_back_v[...])
        real, imag = twist(back[:, :LANES], back[:, LANES:], -1.0)
        conv = mm(inner_back_v[...], jnp.concatenate([real, imag], axis=0))
        return conv.reshape(shape) + signal * skips[order]

    wait_a.wait_recv()
    arrived = recv_a[...].astype(F32)
    signal = smooth(arrived[:, : 2 * OWN], 2)
    signal = smooth(arrived[:, 2 * OWN :], 0) * convolve(signal, 0)
    send_b[...] = convolve(signal, 1).astype(BF16)
    wait_b = exchange(send_b, recv_b, b_sems, row_me, [(p, (p, col_me)) for p in row_peers])
    recv_b[row_me] = send_b[row_me]

    for copy in halo:
        copy.wait_recv()
    x = second_v[...]
    pos = lax.broadcasted_iota(jnp.int32, x.shape, 0)
    head = jnp.where(row_me == 0, 0.0, recv_h[1])
    tail = jnp.where(row_me == rows_n - 1, 0.0, recv_h[0])
    before = jnp.where(pos == 0, head, pltpu.roll(x, 1, 0))
    after = jnp.where(pos == block - 1, tail, pltpu.roll(x, block - 1, 0))
    w = [short_weight[1, j : j + 1, :].astype(F32) for j in range(3)]
    second_v[...] = short_bias[1:2, :] + before * w[0] + x * w[1] + after * w[2]

    wait_b.wait_recv()
    x = recv_b[...].astype(F32).reshape(rows_n // 2, 2, 2 * OWN, LANES)
    early, late = pair(x[:, 0], x[:, 1])
    for j, half in enumerate((early, late)):
        at = slice(j * LANES, (j + 1) * LANES)
        x = half.reshape(LANES, LANES).T * second_v[at, :]
        scale = lax.rsqrt(jnp.mean(x * x, axis=1, keepdims=True) + NORM_EPS)
        x = x * scale * output_gain[...]
        count = LANES // piece
        send_c[j * count : (j + 1) * count] = x.astype(BF16).reshape(count, piece, LANES)
    wait_c = exchange(send_c, recv_c, c_sems, col_me, [(q, (row_me, q)) for q in col_peers])
    recv_c[col_me] = send_c[col_me]
    copies[10].wait()
    wait_c.wait_recv()
    mixed = jnp.concatenate([recv_c[q] for q in range(cols_n)], axis=1)
    step_width = 512
    for start in range(0, out_ref.shape[1], step_width):
        out_ref[:, start : start + step_width] = jnp.dot(
            mixed, out_w_v[:, start : start + step_width], preferred_element_type=F32
        ).astype(BF16)

    for copy in halo + [wait_a, wait_b, wait_c]:
        copy.wait_send()


def local(
    tokens, norm_gain, first_gate, second_gate, value_weight, short_weight, short_bias,
    embed_weight, embed_bias, inner_weight, inner_bias, filter_freq, filter_weight,
    filter_skip, output_gain, output_weight,
):
    rows_n, cols_n = lax.axis_size("row"), lax.axis_size("col")
    block, model = tokens.shape
    piece = block // cols_n
    length = block * rows_n
    width = first_gate.shape[1]
    tables = fast_tables(length)
    out_width = output_weight.shape[1]
    vm = pl.BlockSpec(memory_space=pltpu.VMEM)
    hbm = pl.BlockSpec(memory_space=pl.ANY)
    small = [
        norm_gain.reshape(1, -1),
        short_weight,
        short_bias,
        embed_weight,
        embed_bias.reshape(1, -1),
        inner_weight,
        inner_bias.reshape(1, -1),
        filter_freq.reshape(1, -1),
        filter_weight,
        filter_skip,
        output_gain.reshape(1, -1),
    ]
    operands = [tokens, first_gate, second_gate, value_weight, output_weight, *small, *tables]
    rows_all = 2 * OWN * rows_n
    DMA = pltpu.SemaphoreType.DMA
    return pl.pallas_call(
        functools.partial(fast_kernel, (rows_n, cols_n, block)),
        out_shape=pltpu.VMEM((piece, out_width), BF16),
        in_specs=[hbm] * len(operands),
        out_specs=vm,
        scratch_shapes=[
            pltpu.VMEM(tokens.shape, BF16),
            pltpu.VMEM((3, model, width), BF16),
            pltpu.VMEM(output_weight.shape, BF16),
        ]
        + [pltpu.VMEM(array.shape, array.dtype) for array in small + list(tables)]
        + [
            pltpu.VMEM(tokens.shape, BF16),
            pltpu.VMEM((rows_n, 4 * OWN, LANES), BF16),
            pltpu.VMEM((rows_n, 4 * OWN, LANES), BF16),
            pltpu.VMEM((rows_n, 2 * OWN, LANES), BF16),
            pltpu.VMEM((rows_n, 2 * OWN, LANES), BF16),
            pltpu.VMEM((cols_n, piece, LANES), BF16),
            pltpu.VMEM((cols_n, piece, LANES), BF16),
            pltpu.VMEM((block, width), F32),
            pltpu.VMEM((2, 1, width), F32),
            pltpu.VMEM((2, 1, width), F32),
            pltpu.VMEM((rows_all, 4 * LANES), F32),
            pltpu.VMEM((2, rows_all, 2 * LANES), F32),
            pltpu.VMEM((FEATURE_ROWS, embed_weight.shape[1]), F32),
            DMA((11,)),
            DMA((SMALL,)),
            DMA((2,)),
            DMA((2,)),
            DMA((2,)),
            DMA((2,)),
            DMA((2,)),
        ],
        compiler_params=pltpu.CompilerParams(
            collective_id=0, has_side_effects=True, vmem_limit_bytes=56 * 1024 * 1024
        ),
    )(*operands)


def solution(mesh):
    in_specs = (
        P("row", None),
        P(),
        P(None, "col"),
        P(None, "col"),
        P(None, "col"),
        P(None, None, "col"),
        P(None, "col"),
        P(),
        P(),
        P(),
        P(),
        P(),
        P(None, None, None, ("col", "row")),
        P(None, ("col", "row")),
        P("col"),
        P(),
    )
    out_specs = P(("row", "col"), None)
    return jax.shard_map(local, mesh=mesh, in_specs=in_specs, out_specs=out_specs, check_vma=False)
```

```python
import functools
import math

import jax
import jax.numpy as jnp
import numpy as np
from jax import lax
from jax.experimental import pallas as pl
from jax.experimental.pallas import tpu as pltpu
from jax.sharding import PartitionSpec as P

CHANNELS = 1024
FREQ_BANDS = 16
FEATURES = 33
NORM_EPS = 1e-06
DECAY_TARGET = 0.01
FAST_SPAN = 0.3
SLOW_SPAN = 1.5
LANES = 128
OWN = 4
EARLY_WIDTH = 1024
FEATURE_ROWS = 48
BF16 = jnp.bfloat16
F32 = jnp.float32

SIN_COEFS = (
    6.283185280154403,
    -41.34168061334532,
    81.60247636883796,
    -76.5811726421402,
    39.75982706857711,
)


def fast_tables(length):
    total = 2 * length
    majors = length // LANES
    n1 = np.arange(majors)
    k1 = np.arange(majors) + 0.5
    angle = 2.0 * np.pi * np.outer(k1, n1) / (2 * majors)
    eye = np.eye(OWN)
    inner = np.concatenate([np.kron(np.cos(angle), eye), np.kron(-np.sin(angle), eye)], 0)
    inner_back = inner.T * (2.0 / total)
    n2 = np.arange(LANES)
    turn = np.repeat(2.0 * np.pi * np.outer(k1, n2) / total, OWN, axis=0)
    twiddle = np.stack([np.cos(turn), np.sin(turn)])
    phase = 2.0 * np.pi * (np.outer(n2, n2) % LANES) / LANES
    c, s = np.cos(phase), np.sin(phase)
    outer = np.block([[c, -s], [s, c]])
    ramp = np.linspace(0.0, 1.0, length)
    angles = 2.0 * np.pi * np.arange(length) / length
    bands = np.linspace(0.0001, FREQ_BANDS - 1, FREQ_BANDS)[:, None]
    feats = np.concatenate(
        [ramp[None], np.cos(bands * angles), -np.sin(bands * angles), np.ones((1, length))], 0
    )
    feats = np.pad(feats, ((0, FEATURE_ROWS - feats.shape[0]), (0, 0))).astype(np.float32)
    high = feats.astype(BF16)
    low = (feats - high.astype(np.float32)).astype(BF16)
    return (
        jnp.asarray(inner, BF16),
        jnp.asarray(inner_back, BF16),
        jnp.asarray(twiddle, F32),
        jnp.asarray(outer, BF16),
        jnp.asarray(outer.T, BF16),
        jnp.asarray(np.concatenate([high, low], 0)),
    )


def turn_sin(x):
    d = x - jnp.round(x)
    e = 0.25 - jnp.abs(d)
    q = e * e
    p = SIN_COEFS[4]
    for coef in SIN_COEFS[3::-1]:
        p = coef + q * p
    return e * p


def mm(a, b):
    return jnp.dot(a.astype(BF16), b.astype(BF16), preferred_element_type=F32)


def halves(x):
    high = x.astype(BF16)
    return high, (x - high.astype(F32)).astype(BF16)


def left_three(x):
    high, low = halves(x)
    return jnp.concatenate([high.astype(F32), high.astype(F32), low.astype(F32)], 1).astype(BF16)


def pick(row, start, count):
    shape = (count, row.shape[1])
    want = start + lax.broadcasted_iota(jnp.int32, shape, 0) % OWN
    hit = lax.broadcasted_iota(jnp.int32, shape, 1) == want
    return jnp.sum(jnp.where(hit, row.astype(F32), 0.0), axis=1, keepdims=True)


def column(row):
    count = row.shape[1]
    shape = (count, count)
    hit = lax.broadcasted_iota(jnp.int32, shape, 1) == lax.broadcasted_iota(jnp.int32, shape, 0)
    return jnp.sum(jnp.where(hit, row.astype(F32), 0.0), axis=1, keepdims=True)


def pair(x, y):
    axis = x.ndim - 2
    low = lax.broadcasted_iota(jnp.int32, x.shape, axis) < OWN
    return (
        jnp.where(low, x, pltpu.roll(y, OWN, axis)),
        jnp.where(low, pltpu.roll(x, OWN, axis), y),
    )


SMALL = 11
ROW_MINOR = 4
COL_MINOR = 2


def far_first(me, count, minor):
    major = count // minor
    majors = [lax.rem(lax.div(me, minor) + d, major) * minor for d in range(major)]
    minors = [lax.rem(lax.rem(me, minor) + d, minor) for d in range(minor)]
    offsets = [(a, b) for a in range(major) for b in range(minor) if a or b]
    offsets.sort(key=lambda o: -(min(o[0], major - o[0]) + min(o[1], minor - o[1])))
    return [majors[a] + minors[b] for a, b in offsets]


def fast_kernel(dims, *refs):
    tokens_h, first_h, second_h, value_h, out_w_h = refs[:5]
    small_h = refs[5 : 5 + SMALL]
    inner_h, inner_back_h, twiddle_h, outer_h, outer_back_h, feats_h, out_ref = refs[
        5 + SMALL : 12 + SMALL
    ]
    tokens_v, gates_v, out_w_v = refs[12 + SMALL : 15 + SMALL]
    small_v = refs[15 + SMALL : 15 + 2 * SMALL]
    (
        norm_gain, short_weight, short_bias, embed_weight, embed_bias, inner_weight,
        inner_bias, filter_freq, filter_weight, filter_skip, output_gain,
    ) = small_v
    (
        inner_v, inner_back_v, twiddle_v, outer_v, outer_back_v, feats_v, normed_v,
        send_a, recv_a, send_b, recv_b, send_c, recv_c, second_v, send_h, recv_h,
        taps_v, spectra, embed_pad, load_sem, small_sem, a_sems, b_sems, c_sems,
        send_h_sem, recv_h_sem,
    ) = refs[15 + 2 * SMALL :]
    rows_n, cols_n, block = dims
    length = rows_n * block
    piece = block // cols_n
    row_me = lax.axis_index("row")
    col_me = lax.axis_index("col")
    MESH = pl.DeviceIdType.MESH

    loads = [
        (tokens_h, tokens_v),
        (value_h, gates_v.at[2]),
        (first_h, gates_v.at[0]),
        (second_h, gates_v.at[1]),
        (feats_h, feats_v),
        (inner_h, inner_v),
        (twiddle_h, twiddle_v),
        (outer_h, outer_v),
        (outer_back_h, outer_back_v),
        (inner_back_h, inner_back_v),
        (out_w_h, out_w_v),
    ]
    copies = [
        pltpu.make_async_copy(src, dst, load_sem.at[i]) for i, (src, dst) in enumerate(loads)
    ]
    smalls = [
        pltpu.make_async_copy(src, dst, small_sem.at[i])
        for i, (src, dst) in enumerate(zip(small_h, small_v))
    ]
    row_peers = far_first(row_me, rows_n, ROW_MINOR)
    col_peers = far_first(col_me, cols_n, COL_MINOR)
    barrier = pltpu.get_barrier_semaphore()
    places = [(p, col_me) for p in row_peers] + [(row_me, q) for q in col_peers]

    def greet(some):
        for place in some:
            pl.semaphore_signal(barrier, inc=1, device_id=place, device_id_type=MESH)

    greet(places[:8])
    copies[0].start()
    smalls[0].start()
    copies[1].start()
    copies[2].start()
    greet(places[8:])
    for copy in smalls[1:] + copies[3:10]:
        copy.start()

    def exchange(send, recv, sems, me, places):
        def copy_of(src, dst, place):
            return pltpu.make_async_remote_copy(
                src_ref=src,
                dst_ref=dst,
                send_sem=sems.at[0],
                recv_sem=sems.at[1],
                device_id=place,
                device_id_type=MESH,
            )

        for peer, place in places:
            copy_of(send.at[peer], recv.at[me], place).start()
        count = len(places)
        return copy_of(send.at[pl.ds(0, count)], recv.at[pl.ds(0, count)], places[0][1])

    copies[0].wait()
    smalls[0].wait()
    gain_row = norm_gain[...]
    chunk = 32
    for start in range(0, block, chunk):
        x = tokens_v[start : start + chunk, :].astype(F32)
        scale = lax.rsqrt(jnp.mean(x * x, axis=1, keepdims=True) + NORM_EPS)
        normed_v[start : start + chunk, :] = (x * scale * gain_row).astype(BF16)

    def project(branch):
        return jnp.dot(normed_v[...], gates_v[branch], preferred_element_type=F32)

    def message(gate):
        turned = gate.T
        even, odd = pair(
            turned[:, :LANES].reshape(rows_n // 2, 2 * OWN, LANES),
            turned[:, LANES:].reshape(rows_n // 2, 2 * OWN, LANES),
        )
        return jnp.stack([even, odd], axis=1).reshape(rows_n, 2 * OWN, LANES)

    copies[1].wait()
    send_a[0] = message(project(2)).astype(BF16)
    copies[2].wait()
    send_a[1] = message(project(0)).astype(BF16)
    recv_a[0, row_me] = send_a[0, row_me]
    recv_a[1, row_me] = send_a[1, row_me]

    for copy in smalls[1:]:
        copy.wait()

    pace = filter_freq[...] * (0.5 / math.pi)
    embed_pad[...] = jnp.zeros_like(embed_pad)
    embed_pad[:FEATURES, :] = embed_weight[...] * pace
    embed_pad[FEATURES : FEATURES + 1, :] = embed_bias[...] * pace - 0.25
    embed_left = left_three(embed_pad[...].T)
    inner_left = left_three((inner_weight[...] * pace).T)
    inner_turn = column(inner_bias[...] * pace - 0.25)
    last = jnp.concatenate([filter_weight[o, d] for o in range(2) for d in range(2)], axis=0)
    last_left = left_three(last)
    channels = rows_n * cols_n * OWN
    slowest = math.log(DECAY_TARGET) / SLOW_SPAN
    fastest = math.log(DECAY_TARGET) / FAST_SPAN
    sub = lax.broadcasted_iota(jnp.int32, (2 * OWN, 1), 0)
    channel = ((col_me * rows_n + row_me) * OWN + sub % OWN).astype(F32)
    decay = jnp.abs(slowest + channel * ((fastest - slowest) / (channels - 1)))
    copies[4].wait()
    def filter_part(start, width):
        high = feats_v[:FEATURE_ROWS, start : start + width]
        low = feats_v[FEATURE_ROWS:, start : start + width]
        hidden = turn_sin(
            jnp.dot(
                embed_left,
                jnp.concatenate([high, low, high], 0),
                preferred_element_type=F32,
            )
        )
        high, low = halves(hidden)
        hidden = turn_sin(
            jnp.dot(
                inner_left,
                jnp.concatenate([high, low, high], 0),
                preferred_element_type=F32,
            )
            + inner_turn
        )
        high, low = halves(hidden)
        taps = jnp.dot(
            last_left, jnp.concatenate([high, low, high], 0), preferred_element_type=F32
        )
        lag = start + lax.broadcasted_iota(jnp.int32, (2 * OWN, width), 1)
        window = jnp.exp(-(lag.astype(F32) * (1.0 / (length - 1))) * decay)
        if start == 0:
            window = jnp.where((lag == 0) & (sub >= OWN), 0.0, window)
        for order in range(2):
            x = taps[order * 2 * OWN : (order + 1) * 2 * OWN] * window
            y = pltpu.roll(x, OWN, 0)
            x = jnp.where(sub < OWN, x + y, y - x)
            for m in range(width // (2 * LANES)):
                at = 2 * m * LANES
                plus, minus = pair(x[:, at : at + LANES], x[:, at + LANES : at + 2 * LANES])
                spot = (start // (2 * LANES) + m) * 2 * OWN
                lane = 2 * order * LANES
                taps_v[spot : spot + 2 * OWN, lane : lane + LANES] = plus
                taps_v[spot : spot + 2 * OWN, lane + LANES : lane + 2 * LANES] = minus


    filter_part(0, EARLY_WIDTH)
    pl.semaphore_wait(barrier, rows_n - 1 + cols_n - 1)
    row_places = [(p, (p, col_me)) for p in row_peers]
    wait_a = [
        exchange(send_a.at[i], recv_a.at[i], a_sems.at[i], row_me, row_places) for i in range(2)
    ]
    copies[3].wait()
    gate = project(1).astype(BF16).astype(F32)
    second_v[...] = gate
    send_h[0] = gate[:1]
    send_h[1] = gate[block - 1 :]
    halo = []
    for edge, shift in ((0, rows_n - 1), (1, 1)):
        peer = lax.rem(row_me + shift, rows_n)
        copy = pltpu.make_async_remote_copy(
            src_ref=send_h.at[edge],
            dst_ref=recv_h.at[edge],
            send_sem=send_h_sem.at[edge],
            recv_sem=recv_h_sem.at[edge],
            device_id=(peer, col_me),
            device_id_type=MESH,
        )
        copy.start()
        halo.append(copy)
    copies[10].start()
    filter_part(EARLY_WIDTH, length - EARLY_WIDTH)
    for copy in copies[5:8]:
        copy.wait()
    depth = 2 * OWN * rows_n

    def twist(real, imag, sign):
        cos = twiddle_v[0]
        sin = twiddle_v[1] * sign
        return real * cos + imag * sin, imag * cos - real * sin

    part = mm(inner_v[...], taps_v[...])
    for order in range(2):
        for half in range(2):
            lane = (2 * order + half) * LANES
            real, imag = twist(
                part[:depth, lane : lane + LANES], part[depth:, lane : lane + LANES], 1.0
            )
            spot = slice(half * LANES, (half + 1) * LANES)
            spectra[order, :, spot] = mm(
                jnp.concatenate([real, imag], axis=1), outer_v[:, spot]
            )

    shape = (rows_n, 2 * OWN, LANES)
    low_half = lax.broadcasted_iota(jnp.int32, shape, 1) < OWN
    spot = lax.broadcasted_iota(jnp.int32, shape, 2)
    gap = jnp.zeros((1, 2 * OWN, LANES), F32)

    def smooth(x, branch):
        before = pltpu.roll(x, 1, 2)
        other = pltpu.roll(before, OWN, 1)
        earlier = jnp.concatenate([gap, other[:-1]], 0)
        before = jnp.where(spot == 0, jnp.where(low_half, earlier, other), before)
        after = pltpu.roll(x, LANES - 1, 2)
        other = pltpu.roll(after, OWN, 1)
        later = jnp.concatenate([other[1:], gap], 0)
        after = jnp.where(spot == LANES - 1, jnp.where(low_half, other, later), after)
        w = [pick(short_weight[branch, j : j + 1, :], row_me * OWN, 2 * OWN) for j in range(3)]
        bias = pick(short_bias[branch : branch + 1, :], row_me * OWN, 2 * OWN)
        return bias + before * w[0] + x * w[1] + after * w[2]

    for copy in copies[8:10]:
        copy.wait()
    skips = [pick(filter_skip[order : order + 1, :], 0, 2 * OWN) for order in range(2)]

    def convolve(signal, order):
        part = mm(inner_v[...], signal.reshape(depth, LANES))
        real, imag = twist(part[:depth], part[depth:], 1.0)
        spec = mm(jnp.concatenate([real, imag], axis=1), outer_v[...])
        sr, si = spec[:, :LANES], spec[:, LANES:]
        hr, hi = spectra[order, :, :LANES], spectra[order, :, LANES:]
        prod = jnp.concatenate([sr * hr - si * hi, sr * hi + si * hr], axis=1)
        back = mm(prod, outer_back_v[...])
        real, imag = twist(back[:, :LANES], back[:, LANES:], -1.0)
        conv = mm(inner_back_v[...], jnp.concatenate([real, imag], axis=0))
        return conv.reshape(shape) + signal * skips[order]

    wait_a[0].wait_recv()
    signal = convolve(smooth(recv_a[0].astype(F32), 2), 0)
    wait_a[1].wait_recv()
    signal = smooth(recv_a[1].astype(F32), 0) * signal
    send_b[...] = convolve(signal, 1).astype(BF16)
    wait_b = exchange(send_b, recv_b, b_sems, row_me, row_places)
    recv_b[row_me] = send_b[row_me]

    for copy in halo:
        copy.wait_recv()
    x = second_v[...]
    pos = lax.broadcasted_iota(jnp.int32, x.shape, 0)
    head = jnp.where(row_me == 0, 0.0, recv_h[1])
    tail = jnp.where(row_me == rows_n - 1, 0.0, recv_h[0])
    before = jnp.where(pos == 0, head, pltpu.roll(x, 1, 0))
    after = jnp.where(pos == block - 1, tail, pltpu.roll(x, block - 1, 0))
    w = [short_weight[1, j : j + 1, :].astype(F32) for j in range(3)]
    second_v[...] = short_bias[1:2, :] + before * w[0] + x * w[1] + after * w[2]

    wait_b.wait_recv()
    x = recv_b[...].astype(F32).reshape(rows_n // 2, 2, 2 * OWN, LANES)
    early, late = pair(x[:, 0], x[:, 1])
    for j, half in enumerate((early, late)):
        at = slice(j * LANES, (j + 1) * LANES)
        x = half.reshape(LANES, LANES).T * second_v[at, :]
        scale = lax.rsqrt(jnp.mean(x * x, axis=1, keepdims=True) + NORM_EPS)
        x = x * scale * output_gain[...]
        count = LANES // piece
        send_c[j * count : (j + 1) * count] = x.astype(BF16).reshape(count, piece, LANES)
    wait_c = exchange(send_c, recv_c, c_sems, col_me, [(q, (row_me, q)) for q in col_peers])
    recv_c[col_me] = send_c[col_me]
    copies[10].wait()
    wait_c.wait_recv()
    mixed = jnp.concatenate([recv_c[q] for q in range(cols_n)], axis=1)
    step_width = 512
    for start in range(0, out_ref.shape[1], step_width):
        out_ref[:, start : start + step_width] = jnp.dot(
            mixed, out_w_v[:, start : start + step_width], preferred_element_type=F32
        ).astype(BF16)

    for copy in halo + wait_a + [wait_b, wait_c]:
        copy.wait_send()


def local(
    tokens, norm_gain, first_gate, second_gate, value_weight, short_weight, short_bias,
    embed_weight, embed_bias, inner_weight, inner_bias, filter_freq, filter_weight,
    filter_skip, output_gain, output_weight,
):
    rows_n, cols_n = lax.axis_size("row"), lax.axis_size("col")
    block, model = tokens.shape
    piece = block // cols_n
    length = block * rows_n
    width = first_gate.shape[1]
    tables = fast_tables(length)
    out_width = output_weight.shape[1]
    vm = pl.BlockSpec(memory_space=pltpu.VMEM)
    hbm = pl.BlockSpec(memory_space=pl.ANY)
    small = [
        norm_gain.reshape(1, -1),
        short_weight,
        short_bias,
        embed_weight,
        embed_bias.reshape(1, -1),
        inner_weight,
        inner_bias.reshape(1, -1),
        filter_freq.reshape(1, -1),
        jnp.swapaxes(filter_weight, 2, 3),
        filter_skip,
        output_gain.reshape(1, -1),
    ]
    operands = [tokens, first_gate, second_gate, value_weight, output_weight, *small, *tables]
    rows_all = 2 * OWN * rows_n
    DMA = pltpu.SemaphoreType.DMA
    return pl.pallas_call(
        functools.partial(fast_kernel, (rows_n, cols_n, block)),
        out_shape=pltpu.VMEM((piece, out_width), BF16),
        in_specs=[hbm] * len(operands),
        out_specs=vm,
        scratch_shapes=[
            pltpu.VMEM(tokens.shape, BF16),
            pltpu.VMEM((3, model, width), BF16),
            pltpu.VMEM(output_weight.shape, BF16),
        ]
        + [pltpu.VMEM(array.shape, array.dtype) for array in small + list(tables)]
        + [
            pltpu.VMEM(tokens.shape, BF16),
            pltpu.VMEM((2, rows_n, 2 * OWN, LANES), BF16),
            pltpu.VMEM((2, rows_n, 2 * OWN, LANES), BF16),
            pltpu.VMEM((rows_n, 2 * OWN, LANES), BF16),
            pltpu.VMEM((rows_n, 2 * OWN, LANES), BF16),
            pltpu.VMEM((cols_n, piece, LANES), BF16),
            pltpu.VMEM((cols_n, piece, LANES), BF16),
            pltpu.VMEM((block, width), F32),
            pltpu.VMEM((2, 1, width), F32),
            pltpu.VMEM((2, 1, width), F32),
            pltpu.VMEM((rows_all, 4 * LANES), F32),
            pltpu.VMEM((2, rows_all, 2 * LANES), F32),
            pltpu.VMEM((FEATURE_ROWS, embed_weight.shape[1]), F32),
            DMA((11,)),
            DMA((SMALL,)),
            DMA((2, 2)),
            DMA((2,)),
            DMA((2,)),
            DMA((2,)),
            DMA((2,)),
        ],
        compiler_params=pltpu.CompilerParams(
            collective_id=0, has_side_effects=True, vmem_limit_bytes=56 * 1024 * 1024
        ),
    )(*operands)


def solution(mesh):
    in_specs = (
        P("row", None),
        P(),
        P(None, "col"),
        P(None, "col"),
        P(None, "col"),
        P(None, None, "col"),
        P(None, "col"),
        P(),
        P(),
        P(),
        P(),
        P(),
        P(None, None, None, ("col", "row")),
        P(None, ("col", "row")),
        P("col"),
        P(),
    )
    out_specs = P(("row", "col"), None)
    return jax.shard_map(local, mesh=mesh, in_specs=in_specs, out_specs=out_specs, check_vma=False)
```
